32 devices in a mesh: rep: 2 (over y), fs: 4 (over z), tp: 4 (over x, core).
Axes of the slice: x: 2, y: 2, z: 4, core: 2. Of those that a mesh axis runs over, the one named last changes fastest.
Arguments:
- stream: bfloat16 [4096, 2048], P(('rep', 'fs', 'tp')), may hold values from -6 to 6
- gain_before: float32 [2048], replicated, may hold values from 0.1 to 1.9
- gain_after: float32 [2048], replicated, may hold values from 0.1 to 1.9
- proj_gate: bfloat16 [2048, 3584], P('fs', 'tp'), may hold values from -0.125 to 0.125
- proj_lift: bfloat16 [2048, 3584], P('fs', 'tp'), may hold values from -0.125 to 0.125
- proj_down: bfloat16 [3584, 2048], P('tp', 'fs'), may hold values from -0.09375 to 0.09375
- mixer_gain: float32 [2048], replicated, may hold values from 0.1 to 1.9
- mixer_u: bfloat16 [2048, 2048], P('fs', 'tp'), may hold values from -0.125 to 0.125
- mixer_v: bfloat16 [2048, 2048], P('fs', 'tp'), may hold values from -1 to 1
- layer_gain: float32 [2048], P('tp'), may hold values from 0.1 to 1.9
- layer_shift: float32 [2048], P('tp'), may hold values from -3 to 3
- spatial: bfloat16 [16, 128, 128], P('tp'), may hold values from -0.5 to 0.5
- spatial_shift: float32 [16, 128], P('tp'), may hold values from 0.2 to 2
- mixer_down: bfloat16 [2048, 2048], P('tp', 'fs'), may hold values from -0.125 to 0.125
Outputs:
- result: bfloat16 [4096, 2048], P(('rep', 'fs', 'tp'))
The draws below stay inside these ranges and needn't reach their ends.
All inputs are finite; a program needn't handle non-finite values.
Results may differ from the reference program's by a relative error of at most 0.017.
Values may be sent and summed in bfloat16 or wider, within the bound.
A program may use at most 128 MiB of HBM per device.

```python
import jax
import jax.numpy as jnp
from jax import lax

D = 2048
FF = 3584
GROUPS = 16
GROUP_DIM = 128
SPAN = 128
TOK = 512
A = 2048
TOKENS = 4096
N_TP = 4


def draw_mixer_v(key, part):
    first_key, second_key = jax.random.split(key)
    position = jnp.arange(A, dtype=jnp.float32) / (A - 1)
    rising = 4.0
    basis = jnp.clip(jax.random.normal(first_key, (D, A), jnp.float32), -4.0, 4.0)
    jitter = jnp.exp(jax.random.uniform(second_key, (A,), jnp.float32, -0.3, 0.3))
    column_scale = rising ** (position - 0.5) * jitter
    return jnp.clip(basis * column_scale * D ** (-0.5), -1.0, 1.0).astype(jnp.bfloat16)


def levels(own_key, dims, pieces, low, high):
    def one(dim, blocks):
        draws = jax.random.uniform(jax.random.fold_in(jax.random.fold_in(own_key, 6), dim), (blocks,), jnp.float32, low / len(pieces), high / len(pieces))
        return jnp.repeat(jnp.exp(draws), dims[dim] // blocks).reshape((-1,) + (1,) * (len(dims) - dim - 1))

    factor_of = one(*pieces[0])
    for cut in pieces[1:]:
        factor_of = factor_of * one(*cut)
    return factor_of


def noise(rng, extent, scale, reach, shards=(), kind=jnp.bfloat16):
    result = scale * jax.random.normal(rng, extent, jnp.float32)
    if shards:
        result = result * levels(rng, extent, shards, -0.22, 0.18)
    return jnp.clip(result, -reach, reach).astype(kind)


def setup_inputs(seed: int = 0) -> dict:
    keys = jax.random.split(jax.random.key(seed), 15)
    stream = noise(keys[0], (TOKENS, D), 1.0, 6.0, ((0, 32),))
    gain_before = jnp.clip(1.0 + 0.18 * jax.random.normal(keys[1], (D,), jnp.float32), 0.1, 1.9)
    gain_after = jnp.clip(1.0 + 0.18 * jax.random.normal(keys[2], (D,), jnp.float32), 0.1, 1.9)
    proj_gate = noise(keys[3], (D, FF), D ** -0.5, 0.125, ((0, 4), (1, 4)))
    proj_lift = noise(keys[4], (D, FF), D ** -0.5, 0.125, ((0, 4), (1, 4)))
    proj_down = noise(keys[5], (FF, D), FF ** -0.5, 0.09375, ((0, 4), (1, 4)))
    mixer_gain = jnp.clip(1.0 + 0.18 * jax.random.normal(keys[6], (D,), jnp.float32), 0.1, 1.9)
    mixer_u = noise(keys[7], (D, A), D ** -0.5, 0.125, ((0, 4), (1, 4)))
    mixer_v = draw_mixer_v(jax.random.fold_in(keys[14], 71), 0)
    layer_gain = jnp.clip(1.0 + 0.18 * jax.random.normal(keys[9], (A,), jnp.float32), 0.1, 1.9)
    layer_shift = noise(keys[10], (A,), 0.5, 3.0, ((0, 4),), jnp.float32)
    spatial = noise(keys[11], (GROUPS, SPAN, SPAN), SPAN ** -0.5, 0.5, ((0, 4),))
    spatial_shift = jnp.clip(0.2 + 1.8 * jax.random.uniform(keys[12], (GROUPS, SPAN), jnp.float32) ** levels(keys[12], (GROUPS, SPAN), ((0, 4),), -0.2, 0.2), 0.2, 2.0)
    mixer_down = noise(keys[13], (A, D), A ** -0.5, 0.125, ((0, 4), (1, 4)))
    return {"stream": stream, "gain_before": gain_before, "gain_after": gain_after, "proj_gate": proj_gate, "proj_lift": proj_lift, "proj_down": proj_down, "mixer_gain": mixer_gain, "mixer_u": mixer_u, "mixer_v": mixer_v, "layer_gain": layer_gain, "layer_shift": layer_shift, "spatial": spatial, "spatial_shift": spatial_shift, "mixer_down": mixer_down}


norm_epsilon = 1e-06
layer_epsilon = 1e-05

def norm_rows(row_block, scale_gain):
    widened = row_block.astype(jnp.float32)
    factor = lax.rsqrt(lax.optimization_barrier(jnp.mean(widened * widened, axis=1, keepdims=True)) + norm_epsilon)
    return (widened * factor * scale_gain).astype(jnp.bfloat16)

def blocked_sum(left_rows, right_rows):
    unit_count = left_rows.shape[1] // N_TP
    running = jnp.zeros((left_rows.shape[0], right_rows.shape[1]), jnp.float32)
    for member in range(N_TP):
        partial_value = jnp.dot(left_rows[:, member * unit_count:(member + 1) * unit_count], right_rows[member * unit_count:(member + 1) * unit_count], preferred_element_type=jnp.float32)
        running = running + lax.optimization_barrier(partial_value.astype(jnp.bfloat16)).astype(jnp.float32)
    return running

def half_step(row_block, scale_gain, proj_gate, proj_lift, proj_down):
    normed = norm_rows(row_block, scale_gain)
    gate_vals = jnp.dot(normed, proj_gate, preferred_element_type=jnp.float32)
    lift_vals = jnp.dot(normed, proj_lift, preferred_element_type=jnp.float32)
    hidden = (jax.nn.silu(gate_vals) * lift_vals).astype(jnp.bfloat16)
    delta = blocked_sum(hidden, proj_down)
    return (row_block.astype(jnp.float32) + 0.5 * delta).astype(jnp.bfloat16)

def token_mixer(row_block, mixer_gain, mixer_u, mixer_v, layer_gain, layer_shift, spatial, spatial_shift, mixer_down):
    normed = norm_rows(row_block, mixer_gain)
    u_vals = jnp.dot(normed, mixer_u, preferred_element_type=jnp.float32)
    v_vals = jnp.dot(normed, mixer_v, preferred_element_type=jnp.float32)
    lifted = jax.nn.gelu(v_vals)
    centre = lax.optimization_barrier(jnp.mean(lifted, axis=1, keepdims=True))
    spread = lax.optimization_barrier(jnp.mean(jnp.square(lifted - centre), axis=1, keepdims=True))
    normed_v = ((lifted - centre) * lax.rsqrt(spread + layer_epsilon) * layer_gain + layer_shift).astype(jnp.bfloat16)
    blocked = normed_v.reshape(TOK // SPAN, SPAN, GROUPS, GROUP_DIM).astype(jnp.float32)
    causal = jnp.tril(jnp.ones((SPAN, SPAN), dtype=bool))
    masked = jnp.where(causal[None], spatial.astype(jnp.float32), jnp.float32(0.0))
    mixed_v = jnp.einsum('gts,bsgd->btgd', masked, blocked) + spatial_shift.T[None, :, :, None]
    gated = (jax.nn.gelu(u_vals) * mixed_v.reshape(TOK, GROUPS * GROUP_DIM)).astype(jnp.bfloat16)
    delta = blocked_sum(gated, mixer_down)
    return (row_block.astype(jnp.float32) + delta).astype(jnp.bfloat16)

def reference(stream, gain_before, gain_after, proj_gate, proj_lift, proj_down, mixer_gain, mixer_u, mixer_v, layer_gain, layer_shift, spatial, spatial_shift, mixer_down):

    def one_sequence(row_block):
        first = half_step(row_block, gain_before, proj_gate, proj_lift, proj_down)
        second = token_mixer(first, mixer_gain, mixer_u, mixer_v, layer_gain, layer_shift, spatial, spatial_shift, mixer_down)
        return half_step(second, gain_after, proj_gate, proj_lift, proj_down)
    stacked = stream.reshape(stream.shape[0] // TOK, TOK, stream.shape[1])
    return lax.map(one_sequence, stacked).reshape(stream.shape)
```

```python
import functools

import jax
import jax.numpy as jnp
from jax import lax
from jax.experimental import pallas as pl
from jax.experimental.pallas import tpu as pltpu
from jax.sharding import PartitionSpec as P

SPAN = 128

norm_epsilon = 1e-06
layer_epsilon = 1e-05

MESH = pl.DeviceIdType.MESH
GATE, LIFT, DOWN, MIX_U, MIX_V, MIX_DOWN = range(6)


def norm_rows(widened, scale_gain):
    factor = lax.rsqrt(jnp.mean(widened * widened, axis=1, keepdims=True) + norm_epsilon)
    return (widened * factor * scale_gain).astype(jnp.bfloat16)


def layer_kernel(
    n_rep,
    n_fs,
    n_tp,
    stream,
    gain_before,
    gain_after,
    mixer_gain,
    layer_gain,
    layer_shift,
    spatial,
    spatial_shift,
    proj_gate,
    proj_lift,
    proj_down,
    mixer_u,
    mixer_v,
    mixer_down,
    out,
    gate_all,
    lift_all,
    down_all,
    u_all,
    v_all,
    mix_down_all,
    rows_all,
    to_sibling,
    from_sibling,
    to_chip,
    from_chip,
    partial_all,
    gate_vals,
    hidden,
    u_vals,
    lifted,
    gated,
    mom_own,
    mom_in,
    square,
    resid,
    local_sem,
    z_send,
    z_send_left,
    z_recv,
    y_send,
    y_recv,
    ag_sem,
    agf_sem,
    sib_sem,
    chip_sem,
    mom_sem,
):
    rep, fs, tp = lax.axis_index("rep"), lax.axis_index("fs"), lax.axis_index("tp")
    chip, core = tp // 2, lax.rem(tp, 2)
    n_chip = n_tp // 2
    block, width = stream.shape
    pair = 2 * block
    shards = (proj_gate, proj_lift, proj_down, mixer_u, mixer_v, mixer_down)
    full = (gate_all, lift_all, down_all, u_all, v_all, mix_down_all)
    mine = pl.ds(pl.multiple_of(core * block, block), block)
    theirs = pl.ds(pl.multiple_of((1 - core) * block, block), block)
    sibling = chip * 2 + (1 - core)

    def at(r, f, t):
        return (r, f, t)

    barrier = pltpu.get_barrier_semaphore()

    @pl.when(fs > 0)
    def _():
        pl.semaphore_signal(barrier, inc=1, device_id=at(rep, fs - 1, tp), device_id_type=MESH)

    @pl.when(fs < n_fs - 1)
    def _():
        pl.semaphore_signal(barrier, inc=1, device_id=at(rep, fs + 1, tp), device_id_type=MESH)

    for k in range(1, n_rep):
        pl.semaphore_signal(
            barrier, inc=1, device_id=at(lax.rem(rep + k, n_rep), fs, tp), device_id_type=MESH
        )
    for k in range(1, n_tp):
        pl.semaphore_signal(
            barrier, inc=1, device_id=at(rep, fs, lax.rem(tp + k, n_tp)), device_id_type=MESH
        )

    locals_ = [
        pltpu.make_async_copy(shards[w], full[w].at[fs], local_sem.at[w]) for w in range(6)
    ]
    for copy in locals_:
        copy.start()

    line_peers = jnp.minimum(fs, 1) + jnp.minimum(n_fs - 1 - fs, 1)
    pl.semaphore_wait(barrier, n_rep - 1 + n_tp - 1 + line_peers)

    def piece(w, owner, part):
        rows = full[w].shape[1] // n_rep
        return full[w].at[owner, pl.ds(pl.multiple_of(part * rows, rows), rows)]

    def z_copy(w, owner, step):
        ref = piece(w, owner, rep)
        sem = z_send.at[w, owner] if step > 0 else z_send_left.at[w, owner]
        return pltpu.make_async_remote_copy(
            src_ref=ref, dst_ref=ref, send_sem=sem, recv_sem=z_recv.at[w, owner],
            device_id=at(rep, fs + step, tp), device_id_type=MESH,
        )

    def y_copy(w, owner, k):
        ref = piece(w, owner, rep)
        return pltpu.make_async_remote_copy(
            src_ref=ref, dst_ref=ref, send_sem=y_send.at[w, k - 1, owner],
            recv_sem=y_recv.at[w, k - 1, owner],
            device_id=at(lax.rem(rep + k, n_rep), fs, tp), device_id_type=MESH,
        )

    def own(w):
        locals_[w].wait()

        @pl.when(fs < n_fs - 1)
        def _():
            z_copy(w, fs, 1).start()

        @pl.when(fs > 0)
        def _():
            z_copy(w, fs, -1).start()

    def pump(w):
        def hop(h, carry):
            @pl.when(fs >= h)
            def _():
                z_copy(w, fs - h, 1).wait_recv()
                for k in range(1, n_rep):
                    y_copy(w, fs - h, k).start()

                @pl.when(fs < n_fs - 1)
                def _():
                    z_copy(w, fs - h, 1).start()

            @pl.when(fs + h < n_fs)
            def _():
                z_copy(w, fs + h, -1).wait_recv()
                for k in range(1, n_rep):
                    y_copy(w, fs + h, k).start()

                @pl.when(fs > 0)
                def _():
                    z_copy(w, fs + h, -1).start()

            return carry

        lax.fori_loop(1, n_fs, hop, 0)

    def arrived(w):
        def one(h, carry):
            owner = lax.rem(fs + h, n_fs)
            for k in range(1, n_rep):
                source = lax.rem(rep + n_rep - k, n_rep)
                ref = piece(w, owner, source)
                pltpu.make_async_remote_copy(
                    src_ref=ref, dst_ref=ref, send_sem=y_send.at[w, k - 1, owner],
                    recv_sem=y_recv.at[w, k - 1, owner],
                    device_id=at(source, fs, tp), device_id_type=MESH,
                ).wait_recv()
            return carry

        lax.fori_loop(1, n_fs, one, 0)

    def sends_done():
        def one(owner, carry):
            for w in range(6):
                @pl.when((owner <= fs) & (fs < n_fs - 1))
                def _():
                    z_copy(w, owner, 1).wait_send()

                @pl.when((owner >= fs) & (fs > 0))
                def _():
                    z_copy(w, owner, -1).wait_send()

                @pl.when(owner != fs)
                def _():
                    for k in range(1, n_rep):
                        y_copy(w, owner, k).wait_send()

            return carry

        lax.fori_loop(0, n_fs, one, 0)

    def other_chip(k):
        return lax.rem(chip + k, n_chip)

    def source_chip(k):
        return lax.rem(chip + n_chip - k, n_chip)

    def tp_copy(src, dst, send, recv, target):
        return pltpu.make_async_remote_copy(
            src_ref=src, dst_ref=dst, send_sem=send, recv_sem=recv,
            device_id=at(rep, fs, target), device_id_type=MESH,
        )

    def gather_copy(phase, k):
        ref = rows_all.at[phase, chip, mine]
        target = other_chip(k) * 2 + core
        return tp_copy(ref, ref, ag_sem.at[0, phase, k], ag_sem.at[1, phase, k], target)

    def pass_copy(phase, k):
        ref = rows_all.at[phase, source_chip(k), mine]
        return tp_copy(ref, ref, agf_sem.at[0, phase, k], agf_sem.at[1, phase, k], sibling)

    def gather_start(phase, normed):
        rows_all[phase, chip, mine] = normed
        for k in range(1, n_chip):
            gather_copy(phase, k).start()
        pass_copy(phase, 0).start()

    def gather_pass(phase):
        for k in range(1, n_chip):
            gather_copy(phase, k).wait_recv()
            pass_copy(phase, k).start()

    def gather_end(phase):
        for k in range(1, n_chip):
            gather_copy(phase, k).wait_send()
        for k in range(n_chip):
            pass_copy(phase, k).wait_send()

    def each_pair(compute):
        def one(p, carry):
            compute(p)
            return carry

        lax.fori_loop(0, n_chip, one, 0)

    def sib_copy(phase, p):
        return tp_copy(
            to_sibling.at[phase, p], from_sibling.at[phase, p],
            sib_sem.at[0, phase, p], sib_sem.at[1, phase, p], sibling,
        )

    def chip_copy(phase, k):
        return tp_copy(
            to_chip.at[phase, k - 1], from_chip.at[phase, k - 1],
            chip_sem.at[0, phase, k], chip_sem.at[1, phase, k], other_chip(k) * 2 + core,
        )

    def reduce(phase, left, w):
        cols = full[w].shape[2]

        def product(p):
            def one(f, carry):
                partial_all[f] = jnp.dot(left[p], full[w][f], preferred_element_type=jnp.float32)
                return carry

            lax.fori_loop(0, n_fs, one, 0)
            for f in range(n_fs):
                to_sibling[phase, p, :, f * cols : (f + 1) * cols] = partial_all[f, theirs].astype(
                    jnp.bfloat16
                )
            sib_copy(phase, p).start()

        def joined(p):
            sib_copy(phase, p).wait_recv()
            held = jnp.concatenate([partial_all[f, mine] for f in range(n_fs)], axis=1)
            return held + from_sibling[phase, p].astype(jnp.float32)

        def away(k, carry):
            p = other_chip(k)
            product(p)
            to_chip[phase, k - 1] = joined(p).astype(jnp.bfloat16)
            chip_copy(phase, k).start()
            return carry

        lax.fori_loop(1, n_chip, away, 0)
        product(chip)
        total = joined(chip)
        for k in range(1, n_chip):
            chip_copy(phase, k).wait_recv()
            total = total + from_chip[phase, k - 1].astype(jnp.float32)
        for k in range(1, n_chip):
            chip_copy(phase, k).wait_send()
        for p in range(n_chip):
            sib_copy(phase, p).wait_send()
        return total

    def project(phase, p, w):
        rows = full[w].shape[1]
        total = None
        for f in range(n_fs):
            term = jnp.dot(
                rows_all[phase, p, :, f * rows : (f + 1) * rows], full[w][f],
                preferred_element_type=jnp.float32,
            )
            total = term if total is None else total + term
        return total

    def gate_pair(phase):
        def compute(p):
            gate_vals[p] = project(phase, p, GATE)

        return compute

    def lift_pair(phase):
        def compute(p):
            hidden[p] = (jax.nn.silu(gate_vals[p]) * project(phase, p, LIFT)).astype(jnp.bfloat16)

        return compute

    gather_start(0, norm_rows(stream[...].astype(jnp.float32), gain_before[...]))
    own(GATE)
    own(LIFT)
    pass_copy(0, 0).wait_recv()
    pump(GATE)
    gather_pass(0)
    for k in range(1, n_chip):
        pass_copy(0, k).wait_recv()
    arrived(GATE)
    each_pair(gate_pair(0))
    own(DOWN)
    pump(LIFT)
    arrived(LIFT)
    each_pair(lift_pair(0))
    own(MIX_U)
    pump(DOWN)
    own(MIX_V)
    own(MIX_DOWN)
    arrived(DOWN)
    total = reduce(0, hidden, DOWN)
    first = (stream[...].astype(jnp.float32) + 0.5 * total).astype(jnp.bfloat16)
    resid[...] = first
    gather_end(0)

    gather_start(1, norm_rows(first.astype(jnp.float32), mixer_gain[...]))
    pump(MIX_U)
    pass_copy(1, 0).wait_recv()
    gather_pass(1)
    for k in range(1, n_chip):
        pass_copy(1, k).wait_recv()
    arrived(MIX_U)

    def u_pair(p):
        u_vals[p] = jax.nn.gelu(project(1, p, MIX_U))

    each_pair(u_pair)
    pump(MIX_V)
    arrived(MIX_V)

    def v_pair(p):
        values = jax.nn.gelu(project(1, p, MIX_V))
        lifted[p] = values
        sums = jnp.sum(values, axis=1, keepdims=True)
        squares = jnp.sum(values * values, axis=1, keepdims=True)
        lane = lax.broadcasted_iota(jnp.int32, (pair, 128), 1)
        both = jnp.where(lane == 0, sums, jnp.where(lane == 1, squares, 0.0))
        mom_own[p] = both.T[:8]

    each_pair(v_pair)

    def mom_copy(k):
        return tp_copy(
            mom_own, mom_in.at[k - 1], mom_sem.at[0, k], mom_sem.at[1, k], lax.rem(tp + k, n_tp)
        )

    for k in range(1, n_tp):
        mom_copy(k).start()
    pump(MIX_DOWN)
    square[...] = jnp.zeros_like(square)
    groups = spatial.shape[0]
    square[0:groups, :] = spatial_shift[...]
    shift_columns = square[...].T
    for k in range(1, n_tp):
        mom_copy(k).wait_recv()
    channels = lifted.shape[2]
    group_dim = channels // groups
    all_channels = channels * n_tp

    def mix_pair(p):
        moments = mom_own[p]
        for k in range(1, n_tp):
            moments = moments + mom_in[k - 1, p]
        moments = moments * (1.0 / all_channels)
        columns = jnp.concatenate([moments, jnp.zeros((120, pair), jnp.float32)], axis=0).T
        centre = columns[:, 0:1]
        spread = columns[:, 1:2] - centre * centre
        normed_v = (
            (lifted[p] - centre) * lax.rsqrt(spread + layer_epsilon) * layer_gain[...]
            + layer_shift[...]
        ).astype(jnp.bfloat16)
        row = lax.broadcasted_iota(jnp.int32, (SPAN, SPAN), 0)
        col = lax.broadcasted_iota(jnp.int32, (SPAN, SPAN), 1)
        for g in range(groups):
            masked = jnp.where(row >= col, spatial[g].astype(jnp.float32), 0.0).astype(
                jnp.bfloat16
            )
            cut = slice(g * group_dim, (g + 1) * group_dim)
            for b in range(pair // SPAN):
                span = slice(b * SPAN, (b + 1) * SPAN)
                mixed = jnp.dot(masked, normed_v[span, cut], preferred_element_type=jnp.float32)
                mixed = mixed + shift_columns[:, g : g + 1]
                gated[p, span, cut] = (u_vals[p, span, cut] * mixed).astype(jnp.bfloat16)

    each_pair(mix_pair)
    for k in range(1, n_tp):
        mom_copy(k).wait_send()
    arrived(MIX_DOWN)
    total = reduce(1, gated, MIX_DOWN)
    second = (resid[...].astype(jnp.float32) + total).astype(jnp.bfloat16)
    resid[...] = second
    gather_end(1)

    gather_start(2, norm_rows(second.astype(jnp.float32), gain_after[...]))
    pass_copy(2, 0).wait_recv()
    gate_pair(2)(chip)
    lift_pair(2)(chip)
    gather_pass(2)
    for k in range(1, n_chip):
        pass_copy(2, k).wait_recv()

    def last_pair(k, carry):
        gate_pair(2)(other_chip(k))
        lift_pair(2)(other_chip(k))
        return carry

    lax.fori_loop(1, n_chip, last_pair, 0)
    total = reduce(2, hidden, DOWN)
    out[...] = (resid[...].astype(jnp.float32) + 0.5 * total).astype(jnp.bfloat16)
    gather_end(2)
    sends_done()


def body(
    n_rep,
    n_fs,
    n_tp,
    stream,
    gain_before,
    gain_after,
    proj_gate,
    proj_lift,
    proj_down,
    mixer_gain,
    mixer_u,
    mixer_v,
    layer_gain,
    layer_shift,
    spatial,
    spatial_shift,
    mixer_down,
):
    block, width = stream.shape
    n_chip = n_tp // 2
    pair = 2 * block
    units = proj_gate.shape[1]
    channels = mixer_u.shape[1]
    bf16, f32 = jnp.bfloat16, jnp.float32
    shards = (proj_gate, proj_lift, proj_down, mixer_u, mixer_v, mixer_down)
    vmem = pl.BlockSpec(memory_space=pltpu.VMEM)
    anywhere = pl.BlockSpec(memory_space=pl.ANY)
    dma = pltpu.SemaphoreType.DMA
    spread_reps = max(n_rep - 1, 1)
    spread_chips = max(n_chip - 1, 1)
    return pl.pallas_call(
        functools.partial(layer_kernel, n_rep, n_fs, n_tp),
        out_shape=jax.ShapeDtypeStruct((block, width), bf16),
        in_specs=[vmem] * 8 + [anywhere] * 6,
        out_specs=vmem,
        scratch_shapes=[pltpu.VMEM((n_fs,) + w.shape, bf16) for w in shards]
        + [
            pltpu.VMEM((3, n_chip, pair, width), bf16),
            pltpu.VMEM((3, n_chip, block, width), bf16),
            pltpu.VMEM((3, n_chip, block, width), bf16),
            pltpu.VMEM((3, spread_chips, block, width), bf16),
            pltpu.VMEM((3, spread_chips, block, width), bf16),
            pltpu.VMEM((n_fs, pair, width // n_fs), f32),
            pltpu.VMEM((n_chip, pair, units), f32),
            pltpu.VMEM((n_chip, pair, units), bf16),
            pltpu.VMEM((n_chip, pair, channels), f32),
            pltpu.VMEM((n_chip, pair, channels), f32),
            pltpu.VMEM((n_chip, pair, channels), bf16),
            pltpu.VMEM((n_chip, 8, pair), f32),
            pltpu.VMEM((max(n_tp - 1, 1), n_chip, 8, pair), f32),
            pltpu.VMEM((128, SPAN), f32),
            pltpu.VMEM((block, width), bf16),
            dma((6,)),
            dma((6, n_fs)),
            dma((6, n_fs)),
            dma((6, n_fs)),
            dma((6, spread_reps, n_fs)),
            dma((6, spread_reps, n_fs)),
            dma((2, 3, n_chip)),
            dma((2, 3, n_chip)),
            dma((2, 3, n_chip)),
            dma((2, 3, n_chip)),
            dma((2, n_tp)),
        ],
        compiler_params=pltpu.CompilerParams(
            collective_id=0, has_side_effects=True, vmem_limit_bytes=60 * 1024 * 1024
        ),
    )(
        stream,
        gain_before.reshape(1, -1),
        gain_after.reshape(1, -1),
        mixer_gain.reshape(1, -1),
        layer_gain.reshape(1, -1),
        layer_shift.reshape(1, -1),
        spatial,
        spatial_shift,
        *shards,
    )


def solution(mesh):
    placed = (
        P(("rep", "fs", "tp"), None),
        P(),
        P(),
        P("fs", "tp"),
        P("fs", "tp"),
        P("tp", "fs"),
        P(),
        P("fs", "tp"),
        P("fs", "tp"),
        P("tp"),
        P("tp"),
        P("tp", None, None),
        P("tp", None),
        P("tp", "fs"),
    )
    sizes = (mesh.shape["rep"], mesh.shape["fs"], mesh.shape["tp"])
    return jax.shard_map(
        functools.partial(body, *sizes),
        mesh=mesh,
        in_specs=placed,
        out_specs=P(("rep", "fs", "tp"), None),
        check_vma=False,
    )
```

```python
import functools

import jax
import jax.numpy as jnp
from jax import lax
from jax.experimental import pallas as pl
from jax.experimental.pallas import tpu as pltpu
from jax.sharding import PartitionSpec as P

SPAN = 128

norm_epsilon = 1e-06
layer_epsilon = 1e-05

MESH = pl.DeviceIdType.MESH
GATE, LIFT, DOWN, MIX_U, MIX_V, MIX_DOWN = range(6)
CUTS = 2
AHEAD = 1


def norm_rows(widened, scale_gain):
    factor = lax.rsqrt(jnp.mean(widened * widened, axis=1, keepdims=True) + norm_epsilon)
    return (widened * factor * scale_gain).astype(jnp.bfloat16)


def layer_kernel(
    n_rep,
    n_fs,
    n_tp,
    stream,
    gain_before,
    gain_after,
    mixer_gain,
    layer_gain,
    layer_shift,
    spatial,
    spatial_shift,
    proj_gate,
    proj_lift,
    proj_down,
    mixer_u,
    mixer_v,
    mixer_down,
    out,
    gate_all,
    lift_all,
    down_all,
    u_all,
    v_all,
    mix_down_all,
    rows_all,
    to_sibling,
    from_sibling,
    to_chip,
    from_chip,
    partial_all,
    gate_vals,
    hidden,
    u_vals,
    lifted,
    gated,
    mom_own,
    mom_in,
    square,
    resid,
    local_sem,
    z_send,
    z_send_left,
    z_recv,
    y_send,
    y_recv,
    ag_sem,
    agf_sem,
    sib_sem,
    chip_sem,
    mom_sem,
):
    rep, fs, tp = lax.axis_index("rep"), lax.axis_index("fs"), lax.axis_index("tp")
    chip, core = tp // 2, lax.rem(tp, 2)
    n_chip = n_tp // 2
    block, width = stream.shape
    pair = 2 * block
    shards = (proj_gate, proj_lift, proj_down, mixer_u, mixer_v, mixer_down)
    full = (gate_all, lift_all, down_all, u_all, v_all, mix_down_all)
    mine = pl.ds(pl.multiple_of(core * block, block), block)
    theirs = pl.ds(pl.multiple_of((1 - core) * block, block), block)
    sibling = chip * 2 + (1 - core)

    def at(r, f, t):
        return (r, f, t)

    barrier = pltpu.get_barrier_semaphore()

    @pl.when(fs > 0)
    def _():
        pl.semaphore_signal(barrier, inc=1, device_id=at(rep, fs - 1, tp), device_id_type=MESH)

    @pl.when(fs < n_fs - 1)
    def _():
        pl.semaphore_signal(barrier, inc=1, device_id=at(rep, fs + 1, tp), device_id_type=MESH)

    for k in range(1, n_rep):
        pl.semaphore_signal(
            barrier, inc=1, device_id=at(lax.rem(rep + k, n_rep), fs, tp), device_id_type=MESH
        )
    for k in range(1, n_tp):
        pl.semaphore_signal(
            barrier, inc=1, device_id=at(rep, fs, lax.rem(tp + k, n_tp)), device_id_type=MESH
        )

    locals_ = [
        pltpu.make_async_copy(shards[w], full[w].at[fs], local_sem.at[w]) for w in range(6)
    ]
    for copy in locals_:
        copy.start()

    line_peers = jnp.minimum(fs, 1) + jnp.minimum(n_fs - 1 - fs, 1)
    pl.semaphore_wait(barrier, n_rep - 1 + n_tp - 1 + line_peers)

    items = 6 * CUTS

    def piece(i, owner, part):
        w, cut = i // CUTS, i % CUTS
        rows = full[w].shape[1] // (n_rep * CUTS)
        first_row = pl.multiple_of((part * CUTS + cut) * rows, rows)
        return full[w].at[owner, pl.ds(first_row, rows)]

    def z_copy(i, owner, step):
        ref = piece(i, owner, rep)
        sem = z_send.at[i, owner] if step > 0 else z_send_left.at[i, owner]
        return pltpu.make_async_remote_copy(
            src_ref=ref, dst_ref=ref, send_sem=sem, recv_sem=z_recv.at[i, owner],
            device_id=at(rep, fs + step, tp), device_id_type=MESH,
        )

    def y_copy(i, owner, k):
        ref = piece(i, owner, rep)
        return pltpu.make_async_remote_copy(
            src_ref=ref, dst_ref=ref, send_sem=y_send.at[i, k - 1, owner],
            recv_sem=y_recv.at[i, k - 1, owner],
            device_id=at(lax.rem(rep + k, n_rep), fs, tp), device_id_type=MESH,
        )

    def own(i):
        if i % CUTS == 0:
            locals_[i // CUTS].wait()

        @pl.when(fs < n_fs - 1)
        def _():
            z_copy(i, fs, 1).start()

        @pl.when(fs > 0)
        def _():
            z_copy(i, fs, -1).start()

    def serve(i):
        if i + AHEAD < items:
            own(i + AHEAD)

        def hop(h, carry):
            @pl.when(fs >= h)
            def _():
                z_copy(i, fs - h, 1).wait_recv()

                @pl.when(fs < n_fs - 1)
                def _():
                    z_copy(i, fs - h, 1).start()

                for k in range(1, n_rep):
                    y_copy(i, fs - h, k).start()

            @pl.when(fs + h < n_fs)
            def _():
                z_copy(i, fs + h, -1).wait_recv()

                @pl.when(fs > 0)
                def _():
                    z_copy(i, fs + h, -1).start()

                for k in range(1, n_rep):
                    y_copy(i, fs + h, k).start()

            return carry

        lax.fori_loop(1, n_fs, hop, 0)

    def pump(w):
        for cut in range(CUTS):
            serve(w * CUTS + cut)

    def arrived(w):
        def one(h, carry):
            owner = lax.rem(fs + h, n_fs)
            for cut in range(CUTS):
                i = w * CUTS + cut
                for k in range(1, n_rep):
                    source = lax.rem(rep + n_rep - k, n_rep)
                    ref = piece(i, owner, source)
                    pltpu.make_async_remote_copy(
                        src_ref=ref, dst_ref=ref, send_sem=y_send.at[i, k - 1, owner],
                        recv_sem=y_recv.at[i, k - 1, owner],
                        device_id=at(source, fs, tp), device_id_type=MESH,
                    ).wait_recv()
            return carry

        lax.fori_loop(1, n_fs, one, 0)

    def sends_done():
        def one(owner, carry):
            for i in range(items):
                @pl.when((owner <= fs) & (fs < n_fs - 1))
                def _():
                    z_copy(i, owner, 1).wait_send()

                @pl.when((owner >= fs) & (fs > 0))
                def _():
                    z_copy(i, owner, -1).wait_send()

                @pl.when(owner != fs)
                def _():
                    for k in range(1, n_rep):
                        y_copy(i, owner, k).wait_send()

            return carry

        lax.fori_loop(0, n_fs, one, 0)

    def other_chip(k):
        return lax.rem(chip + k, n_chip)

    def source_chip(k):
        return lax.rem(chip + n_chip - k, n_chip)

    def tp_copy(src, dst, send, recv, target):
        return pltpu.make_async_remote_copy(
            src_ref=src, dst_ref=dst, send_sem=send, recv_sem=recv,
            device_id=at(rep, fs, target), device_id_type=MESH,
        )

    def gather_copy(phase, k):
        ref = rows_all.at[phase, chip, mine]
        target = other_chip(k) * 2 + core
        return tp_copy(ref, ref, ag_sem.at[0, phase, k], ag_sem.at[1, phase, k], target)

    def pass_copy(phase, k):
        ref = rows_all.at[phase, source_chip(k), mine]
        return tp_copy(ref, ref, agf_sem.at[0, phase, k], agf_sem.at[1, phase, k], sibling)

    def gather_start(phase, normed):
        rows_all[phase, chip, mine] = normed
        for k in range(1, n_chip):
            gather_copy(phase, k).start()
        pass_copy(phase, 0).start()

    def gather_pass(phase):
        for k in range(1, n_chip):
            gather_copy(phase, k).wait_recv()
            pass_copy(phase, k).start()

    def gather_end(phase):
        for k in range(1, n_chip):
            gather_copy(phase, k).wait_send()
        for k in range(n_chip):
            pass_copy(phase, k).wait_send()

    def each_pair(compute):
        def one(p, carry):
            compute(p)
            return carry

        lax.fori_loop(0, n_chip, one, 0)

    def sib_copy(phase, p):
        return tp_copy(
            to_sibling.at[phase, p], from_sibling.at[phase, p],
            sib_sem.at[0, phase, p], sib_sem.at[1, phase, p], sibling,
        )

    def chip_copy(phase, k):
        return tp_copy(
            to_chip.at[phase, k - 1], from_chip.at[phase, k - 1],
            chip_sem.at[0, phase, k], chip_sem.at[1, phase, k], other_chip(k) * 2 + core,
        )

    def reduce(phase, left, w, meanwhile=None):
        cols = full[w].shape[2]

        def product(p):
            def one(f, carry):
                partial_all[f] = jnp.dot(left[p], full[w][f], preferred_element_type=jnp.float32)
                return carry

            lax.fori_loop(0, n_fs, one, 0)
            for f in range(n_fs):
                to_sibling[phase, p, :, f * cols : (f + 1) * cols] = partial_all[f, theirs].astype(
                    jnp.bfloat16
                )
            sib_copy(phase, p).start()

        def joined(p):
            sib_copy(phase, p).wait_recv()
            held = jnp.concatenate([partial_all[f, mine] for f in range(n_fs)], axis=1)
            return held + from_sibling[phase, p].astype(jnp.float32)

        def away(k, carry):
            p = other_chip(k)
            product(p)
            to_chip[phase, k - 1] = joined(p).astype(jnp.bfloat16)
            chip_copy(phase, k).start()
            return carry

        lax.fori_loop(1, n_chip, away, 0)
        product(chip)
        total = joined(chip)
        if meanwhile is not None:
            meanwhile()
        for k in range(1, n_chip):
            chip_copy(phase, k).wait_recv()
            total = total + from_chip[phase, k - 1].astype(jnp.float32)
        for k in range(1, n_chip):
            chip_copy(phase, k).wait_send()
        for p in range(n_chip):
            sib_copy(phase, p).wait_send()
        return total

    def project(phase, p, w):
        rows = full[w].shape[1]
        total = None
        for f in range(n_fs):
            term = jnp.dot(
                rows_all[phase, p, :, f * rows : (f + 1) * rows], full[w][f],
                preferred_element_type=jnp.float32,
            )
            total = term if total is None else total + term
        return total

    def gate_pair(phase):
        def compute(p):
            gate_vals[p] = project(phase, p, GATE)

        return compute

    def lift_pair(phase):
        def compute(p):
            hidden[p] = (jax.nn.silu(gate_vals[p]) * project(phase, p, LIFT)).astype(jnp.bfloat16)

        return compute

    gather_start(0, norm_rows(stream[...].astype(jnp.float32), gain_before[...]))
    for i in range(AHEAD):
        own(i)
    pass_copy(0, 0).wait_recv()
    pump(GATE)
    gather_pass(0)
    for k in range(1, n_chip):
        pass_copy(0, k).wait_recv()
    arrived(GATE)
    each_pair(gate_pair(0))
    pump(LIFT)
    arrived(LIFT)
    each_pair(lift_pair(0))
    pump(DOWN)
    arrived(DOWN)
    total = reduce(0, hidden, DOWN, lambda: pump(MIX_U))
    first = (stream[...].astype(jnp.float32) + 0.5 * total).astype(jnp.bfloat16)
    resid[...] = first
    gather_end(0)

    gather_start(1, norm_rows(first.astype(jnp.float32), mixer_gain[...]))
    pump(MIX_V)
    pass_copy(1, 0).wait_recv()
    gather_pass(1)
    for k in range(1, n_chip):
        pass_copy(1, k).wait_recv()
    arrived(MIX_U)

    def u_pair(p):
        u_vals[p] = jax.nn.gelu(project(1, p, MIX_U))

    each_pair(u_pair)
    arrived(MIX_V)

    def v_pair(p):
        values = jax.nn.gelu(project(1, p, MIX_V))
        lifted[p] = values
        sums = jnp.sum(values, axis=1, keepdims=True)
        squares = jnp.sum(values * values, axis=1, keepdims=True)
        lane = lax.broadcasted_iota(jnp.int32, (pair, 128), 1)
        both = jnp.where(lane == 0, sums, jnp.where(lane == 1, squares, 0.0))
        mom_own[p] = both.T[:8]

    each_pair(v_pair)

    def mom_copy(k):
        return tp_copy(
            mom_own, mom_in.at[k - 1], mom_sem.at[0, k], mom_sem.at[1, k], lax.rem(tp + k, n_tp)
        )

    for k in range(1, n_tp):
        mom_copy(k).start()
    pump(MIX_DOWN)
    square[...] = jnp.zeros_like(square)
    groups = spatial.shape[0]
    square[0:groups, :] = spatial_shift[...]
    shift_columns = square[...].T
    for k in range(1, n_tp):
        mom_copy(k).wait_recv()
    channels = lifted.shape[2]
    group_dim = channels // groups
    all_channels = channels * n_tp

    def mix_pair(p):
        moments = mom_own[p]
        for k in range(1, n_tp):
            moments = moments + mom_in[k - 1, p]
        moments = moments * (1.0 / all_channels)
        columns = jnp.concatenate([moments, jnp.zeros((120, pair), jnp.float32)], axis=0).T
        centre = columns[:, 0:1]
        spread = columns[:, 1:2] - centre * centre
        normed_v = (
            (lifted[p] - centre) * lax.rsqrt(spread + layer_epsilon) * layer_gain[...]
            + layer_shift[...]
        ).astype(jnp.bfloat16)
        row = lax.broadcasted_iota(jnp.int32, (SPAN, SPAN), 0)
        col = lax.broadcasted_iota(jnp.int32, (SPAN, SPAN), 1)
        for g in range(groups):
            masked = jnp.where(row >= col, spatial[g].astype(jnp.float32), 0.0).astype(
                jnp.bfloat16
            )
            cut = slice(g * group_dim, (g + 1) * group_dim)
            for b in range(pair // SPAN):
                span = slice(b * SPAN, (b + 1) * SPAN)
                mixed = jnp.dot(masked, normed_v[span, cut], preferred_element_type=jnp.float32)
                mixed = mixed + shift_columns[:, g : g + 1]
                gated[p, span, cut] = (u_vals[p, span, cut] * mixed).astype(jnp.bfloat16)

    each_pair(mix_pair)
    for k in range(1, n_tp):
        mom_copy(k).wait_send()
    arrived(MIX_DOWN)
    total = reduce(1, gated, MIX_DOWN)
    second = (resid[...].astype(jnp.float32) + total).astype(jnp.bfloat16)
    resid[...] = second
    gather_end(1)

    gather_start(2, norm_rows(second.astype(jnp.float32), gain_after[...]))
    pass_copy(2, 0).wait_recv()
    gate_pair(2)(chip)
    lift_pair(2)(chip)
    gather_pass(2)
    for k in range(1, n_chip):
        pass_copy(2, k).wait_recv()

    def last_pair(k, carry):
        gate_pair(2)(other_chip(k))
        lift_pair(2)(other_chip(k))
        return carry

    lax.fori_loop(1, n_chip, last_pair, 0)
    total = reduce(2, hidden, DOWN)
    out[...] = (resid[...].astype(jnp.float32) + 0.5 * total).astype(jnp.bfloat16)
    gather_end(2)
    sends_done()


def body(
    n_rep,
    n_fs,
    n_tp,
    stream,
    gain_before,
    gain_after,
    proj_gate,
    proj_lift,
    proj_down,
    mixer_gain,
    mixer_u,
    mixer_v,
    layer_gain,
    layer_shift,
    spatial,
    spatial_shift,
    mixer_down,
):
    block, width = stream.shape
    n_chip = n_tp // 2
    pair = 2 * block
    units = proj_gate.shape[1]
    channels = mixer_u.shape[1]
    bf16, f32 = jnp.bfloat16, jnp.float32
    shards = (proj_gate, proj_lift, proj_down, mixer_u, mixer_v, mixer_down)
    vmem = pl.BlockSpec(memory_space=pltpu.VMEM)
    anywhere = pl.BlockSpec(memory_space=pl.ANY)
    dma = pltpu.SemaphoreType.DMA
    spread_reps = max(n_rep - 1, 1)
    spread_chips = max(n_chip - 1, 1)
    return pl.pallas_call(
        functools.partial(layer_kernel, n_rep, n_fs, n_tp),
        out_shape=jax.ShapeDtypeStruct((block, width), bf16),
        in_specs=[vmem] * 8 + [anywhere] * 6,
        out_specs=vmem,
        scratch_shapes=[pltpu.VMEM((n_fs,) + w.shape, bf16) for w in shards]
        + [
            pltpu.VMEM((3, n_chip, pair, width), bf16),
            pltpu.VMEM((3, n_chip, block, width), bf16),
            pltpu.VMEM((3, n_chip, block, width), bf16),
            pltpu.VMEM((3, spread_chips, block, width), bf16),
            pltpu.VMEM((3, spread_chips, block, width), bf16),
            pltpu.VMEM((n_fs, pair, width // n_fs), f32),
            pltpu.VMEM((n_chip, pair, units), f32),
            pltpu.VMEM((n_chip, pair, units), bf16),
            pltpu.VMEM((n_chip, pair, channels), f32),
            pltpu.VMEM((n_chip, pair, channels), f32),
            pltpu.VMEM((n_chip, pair, channels), bf16),
            pltpu.VMEM((n_chip, 8, pair), f32),
            pltpu.VMEM((max(n_tp - 1, 1), n_chip, 8, pair), f32),
            pltpu.VMEM((128, SPAN), f32),
            pltpu.VMEM((block, width), bf16),
            dma((6,)),
            dma((6 * CUTS, n_fs)),
            dma((6 * CUTS, n_fs)),
            dma((6 * CUTS, n_fs)),
            dma((6 * CUTS, spread_reps, n_fs)),
            dma((6 * CUTS, spread_reps, n_fs)),
            dma((2, 3, n_chip)),
            dma((2, 3, n_chip)),
            dma((2, 3, n_chip)),
            dma((2, 3, n_chip)),
            dma((2, n_tp)),
        ],
        compiler_params=pltpu.CompilerParams(
            collective_id=0, has_side_effects=True, vmem_limit_bytes=60 * 1024 * 1024
        ),
    )(
        stream,
        gain_before.reshape(1, -1),
        gain_after.reshape(1, -1),
        mixer_gain.reshape(1, -1),
        layer_gain.reshape(1, -1),
        layer_shift.reshape(1, -1),
        spatial,
        spatial_shift,
        *shards,
    )


def solution(mesh):
    placed = (
        P(("rep", "fs", "tp"), None),
        P(),
        P(),
        P("fs", "tp"),
        P("fs", "tp"),
        P("tp", "fs"),
        P(),
        P("fs", "tp"),
        P("fs", "tp"),
        P("tp"),
        P("tp"),
        P("tp", None, None),
        P("tp", None),
        P("tp", "fs"),
    )
    sizes = (mesh.shape["rep"], mesh.shape["fs"], mesh.shape["tp"])
    return jax.shard_map(
        functools.partial(body, *sizes),
        mesh=mesh,
        in_specs=placed,
        out_specs=P(("rep", "fs", "tp"), None),
        check_vma=False,
    )
```
